32 devices in a mesh: fs: 4 (over y, x), tp: 8 (over z, core).
Axes of the slice: x: 2, y: 2, z: 4, core: 2. Of those that a mesh axis runs over, the one named last changes fastest.
Arguments:
- normed: bfloat16 [2048, 12288], P('tp', 'fs'), may hold values from -6 to 6
- key_cot: bfloat16 [2048, 12288], P('tp', 'fs'), may hold values from -6 to 6
- first_map: bfloat16 [2048, 12288], P('tp', 'fs'), may hold values from -6 to 6
- second_map: bfloat16 [2048, 12288], P('tp', 'fs'), may hold values from -6 to 6
- lambdas: float32 [8], replicated, may hold values from 0.3 to 0.8
- factor: bfloat16 [2048, 256], replicated, may hold values from -0.125 to 0.125
- key_master: float32 [2048, 2048], P('fs', 'tp'), may hold values from -0.125 to 0.125
- value_master: float32 [2048, 2048], P('fs', 'tp'), may hold values from -0.125 to 0.125
- key_first: float32 [256, 2048], P('fs', 'tp'), may hold values from -6 to 6
- key_second: float32 [256, 2048], P('fs', 'tp'), may hold values from 0.5 to 2
- value_first: float32 [256, 2048], P('fs', 'tp'), may hold values from -6 to 6
- value_second: float32 [256, 2048], P('fs', 'tp'), may hold values from 0.5 to 2
Outputs:
- key_master_new: float32 [2048, 2048], P('fs', 'tp')
- value_master_new: float32 [2048, 2048], P('fs', 'tp')
- key_copy: bfloat16 [2048, 2048], P(None, 'tp')
- value_copy: bfloat16 [2048, 2048], P(None, 'tp')
- key_first_new: float32 [256, 2048], P('fs', 'tp')
- key_second_new: float32 [256, 2048], P('fs', 'tp')
- value_first_new: float32 [256, 2048], P('fs', 'tp')
- value_second_new: float32 [256, 2048], P('fs', 'tp')
The draws below stay inside these ranges and needn't reach their ends.
All inputs are finite; a program needn't handle non-finite values.
Results may differ from the reference program's by a relative error of at most 0.0012.
Values may be sent and summed in bfloat16 or wider, within the bound.
A program may use at most 64 MiB of HBM per device.

```python
import math
import jax
import jax.numpy as jnp
from jax import lax

D = 2048
HEADS = 8
VALUE_DIM = 256
RANK = 256
TOKENS = 12288
KW = 2048
HV = 2048


def block_levels(rng, extent, cuts, low, high):
    level = 1.0
    for axis_at, shards_of in cuts:
        steps = jax.random.uniform(jax.random.fold_in(jax.random.fold_in(rng, 6), axis_at), (shards_of,), jnp.float32, low / len(cuts), high / len(cuts))
        level = level * jnp.repeat(jnp.exp(steps), extent[axis_at] // shards_of).reshape((-1,) + (1,) * (len(extent) - 1 - axis_at))
    return level


def centred(own_key, shape, width, limit, pieces=(), kind=jnp.bfloat16):
    values = jax.random.normal(own_key, shape, jnp.float32) * width
    if len(pieces) > 0:
        values = block_levels(own_key, shape, pieces, -0.22, 0.18) * values
    return jnp.clip(values, min=-limit, max=limit).astype(kind)


def setup_inputs(seed: int = 0) -> dict:
    splits = jax.random.split(jax.random.key(seed), 13)
    normed = centred(splits[0], (D, TOKENS), 1.0, 6.0, ((0, 8), (1, 4)))
    key_cot = centred(splits[1], (KW, TOKENS), 1.0, 6.0, ((0, 8), (1, 4)))
    first_map = centred(splits[2], (HV, TOKENS), 1.0, 6.0, ((0, 8), (1, 4)))
    second_map = centred(splits[3], (HV, TOKENS), 1.0, 6.0, ((0, 8), (1, 4)))
    lambdas = jnp.clip(jax.random.uniform(splits[4], (HEADS,), jnp.float32, 0.3, 0.8), 0.3, 0.8)
    factor = centred(splits[5], (D, RANK), D ** -0.5, 0.125)
    key_master = centred(splits[6], (D, KW), D ** -0.5, 0.125, ((0, 4), (1, 8)), jnp.float32)
    value_master = centred(splits[7], (D, HV), D ** -0.5, 0.125, ((0, 4), (1, 8)), jnp.float32)
    key_first = centred(splits[8], (RANK, KW), 1.0, 6.0, ((0, 4), (1, 8)), jnp.float32)
    key_second = jnp.clip(jnp.exp(math.log(2.0) - 1.3862944 * jax.random.uniform(splits[9], (RANK, KW), jnp.float32) ** block_levels(splits[9], (RANK, KW), ((0, 4), (1, 8)), -0.2, 0.2)), 0.5, 2.0)
    value_first = centred(splits[10], (RANK, HV), 1.0, 6.0, ((0, 4), (1, 8)), jnp.float32)
    value_second = jnp.clip(jnp.exp(math.log(2.0) - 1.3862944 * jax.random.uniform(splits[11], (RANK, HV), jnp.float32) ** block_levels(splits[11], (RANK, HV), ((0, 4), (1, 8)), -0.2, 0.2)), 0.5, 2.0)
    return dict(normed=normed, key_cot=key_cot, first_map=first_map, second_map=second_map, lambdas=lambdas, factor=factor, key_master=key_master, value_master=value_master, key_first=key_first, key_second=key_second, value_first=value_first, value_second=value_second)


def summed(left, right):
    return lax.dot_general(left, right, (((1,), (1,)), ((), ())), preferred_element_type=jnp.float32)

def advance(gradient, factor32, first, second, master):
    small = lax.dot_general(factor32, gradient, (((0,), (0,)), ((), ())), precision=lax.Precision.HIGHEST)
    first_new = 0.8 * first + 0.2 * small
    second_new = 0.9 * second + 0.1 * small * small
    direction = first_new / (jnp.sqrt(second_new) + 1e-06)
    raw = jnp.dot(factor32, direction, precision=lax.Precision.HIGHEST)
    update = raw / jnp.sqrt(jnp.mean(raw * raw) + 0.01)
    master_new = 0.998 * master - 0.02 * update
    return (master_new, first_new, second_new)

def reference(normed, key_cot, first_map, second_map, lambdas, factor, key_master, value_master, key_first, key_second, value_first, value_second):
    head_lambda = jnp.repeat(lambdas, VALUE_DIM)
    value_cot = (first_map.astype(jnp.float32) - head_lambda[:, None] * second_map.astype(jnp.float32)).astype(jnp.bfloat16)
    norm_scale = 1.0 / jnp.sqrt(jnp.float32(TOKENS))
    key_grad = summed(normed, key_cot) * norm_scale
    value_grad = summed(normed, value_cot) * norm_scale
    factor32 = factor.astype(jnp.float32)
    key_new, key_first_new, key_second_new = advance(key_grad, factor32, key_first, key_second, key_master)
    value_new, value_first_new, value_second_new = advance(value_grad, factor32, value_first, value_second, value_master)
    return (key_new, value_new, key_new.astype(jnp.bfloat16), value_new.astype(jnp.bfloat16), key_first_new, key_second_new, value_first_new, value_second_new)
```

```python
import functools
import math

import jax
import jax.numpy as jnp
from jax import lax
from jax.experimental import pallas as pl
from jax.experimental.pallas import tpu as pltpu
from jax.sharding import PartitionSpec as P

VALUE_DIM = 256
CORES = 2
LANES = 128
LAG = 3
MESH = pl.DeviceIdType.MESH
F32 = jnp.float32
BF16 = jnp.bfloat16


def flipped(index, bit):
    step = 1 << bit
    return index + step * (1 - 2 * ((index // step) % 2))


def split(value):
    high = value.astype(BF16)
    return high, (value - high.astype(F32)).astype(BF16)


def kernel(
    n_fs,
    n_tp,
    scale,
    normed,
    key_cot,
    first_map,
    second_map,
    lambdas,
    factor,
    key_master,
    value_master,
    key_first,
    key_second,
    value_first,
    value_second,
    key_new,
    value_new,
    key_copy,
    value_copy,
    key_first_new,
    key_second_new,
    value_first_new,
    value_second_new,
    x_v,
    kc_v,
    vc_v,
    sm_v,
    fac_v,
    ft_v,
    mom_v,
    own,
    away,
    sib,
    left,
    right,
    right_out,
    proj,
    key_acc,
    value_acc,
    masters,
    raw,
    copies,
    part,
    part_in,
    moved,
    dirs,
    norms,
    in_sem,
    sib_s,
    sib_r,
    left_s,
    left_r,
    right_s,
    right_r,
    proj_s,
    proj_r,
    mast_s,
    mast_r,
    part_s,
    part_r,
    dir_s,
    dir_r,
    norm_s,
    norm_r,
    out_sem,
):
    fs = lax.axis_index("fs")
    tp = lax.axis_index("tp")
    z = tp // CORES
    core = tp % CORES
    n_z = n_tp // CORES
    features = normed.shape[0]
    width = first_map.shape[0]
    rank = factor.shape[1]
    pieces = own.shape[0]
    subs, sub_rows = left.shape[0] // pieces, left.shape[1]
    steps = pieces * subs
    fs_rows = key_master.shape[0]
    rank_rows = rank // n_fs
    bits = n_fs.bit_length() - 1
    other = z * CORES + (1 - core)

    loads = [
        pltpu.make_async_copy(normed, x_v, in_sem.at[0]),
        pltpu.make_async_copy(factor, fac_v, in_sem.at[1]),
        pltpu.make_async_copy(first_map, vc_v, in_sem.at[2]),
        pltpu.make_async_copy(second_map, sm_v, in_sem.at[3]),
        pltpu.make_async_copy(key_cot, kc_v, in_sem.at[4]),
        pltpu.make_async_copy(key_master, masters.at[0, fs], in_sem.at[5]),
        pltpu.make_async_copy(value_master, masters.at[1, fs], in_sem.at[6]),
        pltpu.make_async_copy(key_first, mom_v.at[0], in_sem.at[7]),
        pltpu.make_async_copy(value_first, mom_v.at[1], in_sem.at[8]),
        pltpu.make_async_copy(key_second, mom_v.at[2], in_sem.at[9]),
        pltpu.make_async_copy(value_second, mom_v.at[3], in_sem.at[10]),
    ]
    for load in loads:
        load.start()

    barrier = pltpu.get_barrier_semaphore()
    for d in range(1, n_fs):
        pl.semaphore_signal(
            barrier, inc=1, device_id=(lax.rem(fs + d, n_fs), tp), device_id_type=MESH
        )
    for d in range(1, n_tp):
        pl.semaphore_signal(
            barrier, inc=1, device_id=(fs, lax.rem(tp + d, n_tp)), device_id_type=MESH
        )
    pl.semaphore_wait(barrier, n_fs + n_tp - 2)

    def master_copy(kv, step, j):
        order = list(range(bits)) if kv == 0 else list(range(bits))[::-1]
        block = fs
        for t in range(step):
            if (j >> t) & 1:
                block = flipped(block, order[t])
        if j == 0:
            src = (key_master, value_master)[kv]
        else:
            src = masters.at[kv, block]
        slot = (1 << step) - 1 + j
        return pltpu.make_async_remote_copy(
            src_ref=src,
            dst_ref=masters.at[kv, block],
            send_sem=mast_s.at[kv, slot],
            recv_sem=mast_r.at[kv, slot],
            device_id=(flipped(fs, order[step]), tp),
            device_id_type=MESH,
        )

    for step in range(bits):
        for kv in range(2):
            master_copy(kv, step, 0).start()

    def wait_masters(step):
        for kv in range(2):
            for j in range(1 << step):
                master_copy(kv, step, j).wait_recv()

    def sib_copy(k):
        return pltpu.make_async_remote_copy(
            src_ref=away.at[k],
            dst_ref=sib.at[k],
            send_sem=sib_s.at[k],
            recv_sem=sib_r.at[k],
            device_id=(fs, other),
            device_id_type=MESH,
        )

    def left_copy(s):
        return pltpu.make_async_remote_copy(
            src_ref=left.at[s],
            dst_ref=left.at[s],
            send_sem=left_s.at[s],
            recv_sem=left_r.at[s],
            device_id=(fs, lax.rem(tp + CORES, n_tp)),
            device_id_type=MESH,
        )

    def right_copy(s):
        return pltpu.make_async_remote_copy(
            src_ref=right_out.at[s],
            dst_ref=right.at[s],
            send_sem=right_s.at[s],
            recv_sem=right_r.at[s],
            device_id=(fs, lax.rem(tp + n_tp - CORES, n_tp)),
            device_id_type=MESH,
        )

    def proj_copy(k):
        return pltpu.make_async_remote_copy(
            src_ref=proj.at[core * pieces + k],
            dst_ref=proj.at[core * pieces + k],
            send_sem=proj_s.at[k],
            recv_sem=proj_r.at[k],
            device_id=(fs, other),
            device_id_type=MESH,
        )

    loads[0].wait()
    loads[1].wait()
    ft_v[...] = fac_v[pl.ds(pl.multiple_of(tp * features, features), features), :].astype(F32).T.astype(BF16)

    def project(side, k):
        cols = pl.ds(pl.multiple_of((side * pieces + k) * LANES, LANES), LANES)
        return jnp.dot(ft_v[...], x_v[:, cols], preferred_element_type=F32)

    @pl.loop(0, pieces)
    def _(k):
        away[k] = project(1 - core, k)
        sib_copy(k).start()
        own[k] = project(core, k)

    loads[2].wait()
    loads[3].wait()
    span = math.gcd(width, VALUE_DIM)
    for b in range(width // span):
        row_lambda = lambdas[(tp * width + b * span) // VALUE_DIM]

        @pl.loop(0, vc_v.shape[1] // LANES)
        def _(c):
            at = (pl.ds(b * span, span), pl.ds(pl.multiple_of(c * LANES, LANES), LANES))
            vc_v[at] = (vc_v[at].astype(F32) - row_lambda * sm_v[at].astype(F32)).astype(BF16)

    loads[4].wait()
    key_acc[...] = jnp.zeros_like(key_acc)
    value_acc[...] = jnp.zeros_like(value_acc)

    def accumulate(piece):
        cols = pl.ds(pl.multiple_of(piece * LANES, LANES), LANES)
        dims = (((1,), (1,)), ((), ()))
        key_acc[...] += lax.dot_general(
            proj[piece], kc_v[:, cols], dims, preferred_element_type=F32
        )
        value_acc[...] += lax.dot_general(
            proj[piece], vc_v[:, cols], dims, preferred_element_type=F32
        )

    def sibling_piece(k):
        return (1 - core) * pieces + k

    def accumulate_sibling(k):
        pltpu.make_async_remote_copy(
            src_ref=proj.at[sibling_piece(k)],
            dst_ref=proj.at[sibling_piece(k)],
            send_sem=proj_s.at[k],
            recv_sem=proj_r.at[k],
            device_id=(fs, other),
            device_id_type=MESH,
        ).wait_recv()
        accumulate(sibling_piece(k))

    def rows_of(s):
        return pl.ds(pl.multiple_of((s % subs) * sub_rows, sub_rows), sub_rows)

    @pl.loop(0, steps + LAG * (n_z - 1))
    def _(i):
        @pl.when(jnp.logical_and(i < steps, i % subs == 0))
        def _():
            k = i // subs
            sib_copy(k).wait_recv()
            own[k] = own[k] + sib[k]

        s_left = i - LAG * z

        @pl.when(jnp.logical_and(s_left >= 0, s_left < steps))
        def _():
            total = own[s_left // subs, rows_of(s_left), :]

            @pl.when(z > 0)
            def _():
                left_copy(s_left).wait_recv()
                left[s_left] = left[s_left] + total

            @pl.when(z == 0)
            def _():
                left[s_left] = total

            @pl.when(z < n_z - 1)
            def _():
                left_copy(s_left).start()

        s_right = i - LAG * (n_z - 1 - z)

        @pl.when(jnp.logical_and(s_right >= 0, s_right < steps))
        def _():
            total = own[s_right // subs, rows_of(s_right), :]

            @pl.when(z < n_z - 1)
            def _():
                right_copy(s_right).wait_recv()

                @pl.when(z > 0)
                def _():
                    right_out[s_right] = right[s_right] + total

            @pl.when(z == n_z - 1)
            def _():
                right[s_right] = jnp.zeros_like(total)

                @pl.when(z > 0)
                def _():
                    right_out[s_right] = total

            @pl.when(z > 0)
            def _():
                right_copy(s_right).start()

        s_done = i - LAG * jnp.maximum(z, n_z - 1 - z)

        @pl.when(jnp.logical_and(s_done >= 0, s_done < steps))
        def _():
            k = s_done // subs
            mine = core * pieces + k
            high, low = split(left[s_done] + right[s_done])
            proj[mine, rows_of(s_done), :] = high
            proj[mine, pl.ds(pl.multiple_of(rank + (s_done % subs) * sub_rows, sub_rows), sub_rows), :] = low

            @pl.when(s_done % subs == subs - 1)
            def _():
                proj_copy(k).start()
                accumulate(mine)

                @pl.when(k > 0)
                def _():
                    accumulate_sibling(k - 1)

        for t in range(1, bits):

            @pl.when(i == (steps * t) // bits)
            def _():
                wait_masters(t - 1)
                for j in range(1, 1 << t):
                    for kv in range(2):
                        master_copy(kv, t, j).start()

    accumulate_sibling(pieces - 1)

    for j in range(n_fs):
        rows = pl.ds(j * rank_rows, rank_rows)
        lows = pl.ds(rank + j * rank_rows, rank_rows)
        part[j, 0] = (key_acc[rows, :] + key_acc[lows, :]) * scale
        part[j, 1] = (value_acc[rows, :] + value_acc[lows, :]) * scale

    def part_copy(d):
        to = lax.rem(fs + d, n_fs)
        return pltpu.make_async_remote_copy(
            src_ref=part.at[to],
            dst_ref=part_in.at[d - 1],
            send_sem=part_s.at[d - 1],
            recv_sem=part_r.at[d - 1],
            device_id=(to, tp),
            device_id_type=MESH,
        )

    def dir_copy(d):
        return pltpu.make_async_remote_copy(
            src_ref=dirs.at[fs],
            dst_ref=dirs.at[fs],
            send_sem=dir_s.at[d - 1],
            recv_sem=dir_r.at[d - 1],
            device_id=(lax.rem(fs + d, n_fs), tp),
            device_id_type=MESH,
        )

    def norm_copy(d):
        return pltpu.make_async_remote_copy(
            src_ref=norms.at[0],
            dst_ref=norms.at[d],
            send_sem=norm_s.at[d - 1],
            recv_sem=norm_r.at[d - 1],
            device_id=(fs, lax.rem(tp + d, n_tp)),
            device_id_type=MESH,
        )

    for d in range(1, n_fs):
        part_copy(d).start()
    for load in loads[7:]:
        load.wait()
    small = part[fs]
    for d in range(1, n_fs):
        part_copy(d).wait_recv()
        small = small + part_in[d - 1]
    first_new = 0.8 * mom_v[0:2] + 0.2 * small
    second_new = 0.9 * mom_v[2:4] + 0.1 * small * small
    dirs[fs] = first_new / (jnp.sqrt(second_new) + 1e-06)
    for d in range(1, n_fs):
        dir_copy(d).start()
    moved[0:2] = first_new
    moved[2:4] = second_new
    moments = [
        pltpu.make_async_copy(moved.at[n], ref, out_sem.at[n])
        for n, ref in enumerate((key_first_new, value_first_new, key_second_new, value_second_new))
    ]
    for copy in moments:
        copy.start()
    for load in loads[5:7]:
        load.wait()
    for d in range(1, n_fs):
        pltpu.make_async_remote_copy(
            src_ref=dirs.at[lax.rem(fs + n_fs - d, n_fs)],
            dst_ref=dirs.at[lax.rem(fs + n_fs - d, n_fs)],
            send_sem=dir_s.at[d - 1],
            recv_sem=dir_r.at[d - 1],
            device_id=(lax.rem(fs + d, n_fs), tp),
            device_id_type=MESH,
        ).wait_recv()

    block = fs_rows
    sums = []
    for kv in range(2):
        high, low = split(jnp.concatenate([dirs[j, kv] for j in range(n_fs)], axis=0))

        def body(n, total):
            rows = fac_v[pl.ds(pl.multiple_of(n * block, block), block), :]
            out = jnp.dot(rows, high, preferred_element_type=F32) + jnp.dot(
                rows, low, preferred_element_type=F32
            )
            raw[kv, n] = out
            return total + jnp.sum((out * out).reshape(block // 8, 8, width), axis=0)

        total = lax.fori_loop(0, n_fs, body, jnp.zeros((8, width), F32))
        sums.append(jnp.sum(total))
    norms[0, 0] = jnp.full(norms.shape[2:], sums[0], F32)
    norms[0, 1] = jnp.full(norms.shape[2:], sums[1], F32)
    for d in range(1, n_tp):
        norm_copy(d).start()
    wait_masters(bits - 1)
    squares = norms[0]
    for d in range(1, n_tp):
        norm_copy(d).wait_recv()
        squares = squares + norms[d]
    cells = factor.shape[0] * width * n_tp
    factors = 0.02 / jnp.sqrt(squares / cells + 0.01)

    def copy_out(kv, n):
        rows = pl.ds(pl.multiple_of(n * block, block), block)
        return pltpu.make_async_copy(
            copies.at[kv, n], (key_copy, value_copy)[kv].at[rows, :], out_sem.at[4 + kv * (n_fs + 1) + n]
        )

    def new_out(kv):
        return pltpu.make_async_copy(
            raw.at[kv, fs], (key_new, value_new)[kv], out_sem.at[4 + kv * (n_fs + 1) + n_fs]
        )

    for kv in range(2):
        grain = factors[kv, 0:1, 0:1]

        @pl.loop(0, n_fs)
        def _(n):
            new = 0.998 * masters[kv, n] - grain * raw[kv, n]
            raw[kv, n] = new
            copies[kv, n] = new.astype(BF16)
            copy_out(kv, n).start()

        new_out(kv).start()

    @pl.loop(0, pieces)
    def _(k):
        sib_copy(k).wait_send()
        proj_copy(k).wait_send()

    @pl.loop(0, steps)
    def _(s):
        @pl.when(z < n_z - 1)
        def _():
            left_copy(s).wait_send()

        @pl.when(z > 0)
        def _():
            right_copy(s).wait_send()

    for kv in range(2):
        for step in range(bits):
            for j in range(1 << step):
                master_copy(kv, step, j).wait_send()
    for d in range(1, n_fs):
        part_copy(d).wait_send()
        dir_copy(d).wait_send()
    for d in range(1, n_tp):
        norm_copy(d).wait_send()
    for copy in moments:
        copy.wait()
    for kv in range(2):
        for n in range(n_fs):
            copy_out(kv, n).wait()
        new_out(kv).wait()


def local(n_fs, n_tp, *args):
    normed, key_cot, first_map, second_map, lambdas, factor, key_master = args[:7]
    features, tokens = normed.shape
    width = first_map.shape[0]
    rows, rank = factor.shape
    fs_rows = key_master.shape[0]
    rank_rows = rank // n_fs
    pieces = tokens // (CORES * LANES)
    subs = 2
    steps = pieces * subs
    sub_rows = rank // subs
    scale = 1.0 / math.sqrt(tokens * n_fs)
    any_spec = pl.BlockSpec(memory_space=pl.ANY)
    specs = [any_spec] * 12
    specs[4] = pl.BlockSpec(memory_space=pltpu.SMEM)
    dma = pltpu.SemaphoreType.DMA
    sds = jax.ShapeDtypeStruct
    small = sds((rank_rows, width), F32)
    return pl.pallas_call(
        functools.partial(kernel, n_fs, n_tp, scale),
        out_shape=[
            sds((fs_rows, width), F32),
            sds((fs_rows, width), F32),
            sds((rows, width), BF16),
            sds((rows, width), BF16),
            small,
            small,
            small,
            small,
        ],
        in_specs=specs,
        out_specs=[any_spec] * 8,
        scratch_shapes=[
            pltpu.VMEM((features, tokens), BF16),
            pltpu.VMEM((width, tokens), BF16),
            pltpu.VMEM((width, tokens), BF16),
            pltpu.VMEM((width, tokens), BF16),
            pltpu.VMEM((rows, rank), BF16),
            pltpu.VMEM((rank, features), BF16),
            pltpu.VMEM((4, rank_rows, width), F32),
            pltpu.VMEM((pieces, rank, LANES), F32),
            pltpu.VMEM((pieces, rank, LANES), F32),
            pltpu.VMEM((pieces, rank, LANES), F32),
            pltpu.VMEM((steps, sub_rows, LANES), F32),
            pltpu.VMEM((steps, sub_rows, LANES), F32),
            pltpu.VMEM((steps, sub_rows, LANES), F32),
            pltpu.VMEM((CORES * pieces, 2 * rank, LANES), BF16),
            pltpu.VMEM((2 * rank, width), F32),
            pltpu.VMEM((2 * rank, width), F32),
            pltpu.VMEM((2, n_fs, fs_rows, width), F32),
            pltpu.VMEM((2, n_fs, fs_rows, width), F32),
            pltpu.VMEM((2, n_fs, fs_rows, width), BF16),
            pltpu.VMEM((n_fs, 2, rank_rows, width), F32),
            pltpu.VMEM((n_fs - 1, 2, rank_rows, width), F32),
            pltpu.VMEM((4, rank_rows, width), F32),
            pltpu.VMEM((n_fs, 2, rank_rows, width), F32),
            pltpu.VMEM((n_tp, 2, 8, LANES), F32),
            dma((11,)),
            dma((pieces,)),
            dma((pieces,)),
            dma((steps,)),
            dma((steps,)),
            dma((steps,)),
            dma((steps,)),
            dma((pieces,)),
            dma((pieces,)),
            dma((2, n_fs - 1)),
            dma((2, n_fs - 1)),
            dma((n_fs - 1,)),
            dma((n_fs - 1,)),
            dma((n_fs - 1,)),
            dma((n_fs - 1,)),
            dma((n_tp - 1,)),
            dma((n_tp - 1,)),
            dma((4 + 2 * (n_fs + 1),)),
        ],
        compiler_params=pltpu.CompilerParams(
            collective_id=0, has_side_effects=True, vmem_limit_bytes=60 * 1024 * 1024
        ),
    )(*args)


def solution(mesh):
    in_specs = (
        P("tp", "fs"),
        P("tp", "fs"),
        P("tp", "fs"),
        P("tp", "fs"),
        P(),
        P(),
        P("fs", "tp"),
        P("fs", "tp"),
        P("fs", "tp"),
        P("fs", "tp"),
        P("fs", "tp"),
        P("fs", "tp"),
    )
    out_specs = (
        P("fs", "tp"),
        P("fs", "tp"),
        P(None, "tp"),
        P(None, "tp"),
        P("fs", "tp"),
        P("fs", "tp"),
        P("fs", "tp"),
        P("fs", "tp"),
    )
    body = functools.partial(local, mesh.shape["fs"], mesh.shape["tp"])

    def ordered(*args):
        out = body(*args)
        return tuple(out)

    return jax.shard_map(ordered, mesh=mesh, in_specs=in_specs, out_specs=out_specs, check_vma=False)
```

```python
import functools
import math

import jax
import jax.numpy as jnp
from jax import lax
from jax.experimental import pallas as pl
from jax.experimental.pallas import tpu as pltpu
from jax.sharding import PartitionSpec as P

VALUE_DIM = 256
CORES = 2
LANES = 128
TOKENS_AT_ONCE = 256
LAG = 3
MESH = pl.DeviceIdType.MESH
F32 = jnp.float32
BF16 = jnp.bfloat16


def flipped(index, bit):
    step = 1 << bit
    return index + step * (1 - 2 * ((index // step) % 2))


def split(value):
    high = value.astype(BF16)
    return high, (value - high.astype(F32)).astype(BF16)


def kernel(
    n_fs,
    n_tp,
    scale,
    normed,
    key_cot,
    first_map,
    second_map,
    lambdas,
    factor,
    key_master,
    value_master,
    key_first,
    key_second,
    value_first,
    value_second,
    masters,
    raw_out,
    moved_out,
    factors_out,
    x_v,
    kc_v,
    vc_v,
    sm_v,
    fac_v,
    ft32,
    ft_v,
    mom_v,
    own,
    away,
    sib,
    left,
    right,
    right_out,
    proj,
    key_acc,
    value_acc,
    raw,
    grain_v,
    part,
    part_in,
    moved,
    dirs,
    norms,
    in_sem,
    sib_s,
    sib_r,
    left_s,
    left_r,
    right_s,
    right_r,
    proj_s,
    proj_r,
    mast_s,
    mast_r,
    part_s,
    part_r,
    dir_s,
    dir_r,
    norm_s,
    norm_r,
    out_sem,
):
    fs = lax.axis_index("fs")
    tp = lax.axis_index("tp")
    z = tp // CORES
    core = tp % CORES
    n_z = n_tp // CORES
    features = normed.shape[0]
    width = first_map.shape[0]
    rank = factor.shape[1]
    groups, pieces, group_rows, tile = own.shape
    steps = groups * pieces
    group_fs = group_rows // n_fs
    fs_rows = key_master.shape[0]
    rank_rows = rank // n_fs
    bits = n_fs.bit_length() - 1
    other = z * CORES + (1 - core)

    loads = [
        pltpu.make_async_copy(normed, x_v, in_sem.at[0]),
        pltpu.make_async_copy(factor, fac_v, in_sem.at[1]),
        pltpu.make_async_copy(first_map, vc_v, in_sem.at[2]),
        pltpu.make_async_copy(second_map, sm_v, in_sem.at[3]),
        pltpu.make_async_copy(key_cot, kc_v, in_sem.at[4]),
        pltpu.make_async_copy(key_first, mom_v.at[0], in_sem.at[5]),
        pltpu.make_async_copy(value_first, mom_v.at[1], in_sem.at[6]),
        pltpu.make_async_copy(key_second, mom_v.at[2], in_sem.at[7]),
        pltpu.make_async_copy(value_second, mom_v.at[3], in_sem.at[8]),
    ]
    for load in loads:
        load.start()

    barrier = pltpu.get_barrier_semaphore()
    for d in range(1, n_fs):
        pl.semaphore_signal(
            barrier, inc=1, device_id=(lax.rem(fs + d, n_fs), tp), device_id_type=MESH
        )
    for d in range(1, n_tp):
        pl.semaphore_signal(
            barrier, inc=1, device_id=(fs, lax.rem(tp + d, n_tp)), device_id_type=MESH
        )
    pl.semaphore_wait(barrier, n_fs + n_tp - 2)

    def master_copy(kv, step, j):
        order = list(range(bits)) if kv == 0 else list(range(bits))[::-1]
        block = fs
        for t in range(step):
            if (j >> t) & 1:
                block = flipped(block, order[t])
        if j == 0:
            src = (key_master, value_master)[kv]
        else:
            src = masters.at[kv, block]
        slot = (1 << step) - 1 + j
        return pltpu.make_async_remote_copy(
            src_ref=src,
            dst_ref=masters.at[kv, block],
            send_sem=mast_s.at[kv, slot],
            recv_sem=mast_r.at[kv, slot],
            device_id=(flipped(fs, order[step]), tp),
            device_id_type=MESH,
        )

    for step in range(bits):
        for kv in range(2):
            master_copy(kv, step, 0).start()

    def wait_masters(step):
        for kv in range(2):
            for j in range(1 << step):
                master_copy(kv, step, j).wait_recv()

    def sib_copy(k):
        return pltpu.make_async_remote_copy(
            src_ref=away.at[:, k],
            dst_ref=sib.at[:, k],
            send_sem=sib_s.at[k],
            recv_sem=sib_r.at[k],
            device_id=(fs, other),
            device_id_type=MESH,
        )

    def left_copy(s):
        return pltpu.make_async_remote_copy(
            src_ref=left.at[s],
            dst_ref=left.at[s],
            send_sem=left_s.at[s],
            recv_sem=left_r.at[s],
            device_id=(fs, lax.rem(tp + CORES, n_tp)),
            device_id_type=MESH,
        )

    def right_copy(s):
        return pltpu.make_async_remote_copy(
            src_ref=right_out.at[s],
            dst_ref=right.at[s],
            send_sem=right_s.at[s],
            recv_sem=right_r.at[s],
            device_id=(fs, lax.rem(tp + n_tp - CORES, n_tp)),
            device_id_type=MESH,
        )

    def proj_copy(s, side):
        at = proj.at[s // pieces, side * pieces + s % pieces]
        return pltpu.make_async_remote_copy(
            src_ref=at,
            dst_ref=at,
            send_sem=proj_s.at[s],
            recv_sem=proj_r.at[s],
            device_id=(fs, other),
            device_id_type=MESH,
        )

    loads[0].wait()
    loads[1].wait()
    turned = fac_v[pl.ds(pl.multiple_of(tp * features, features), features), :].astype(F32).T
    for g in range(groups):
        for j in range(n_fs):
            row = j * rank_rows + g * group_fs
            at = g * group_rows + j * group_fs
            ft32[at : at + group_fs, :] = turned[row : row + group_fs, :]
    ft_v[...] = ft32[...].astype(BF16)

    def tokens_of(side, k):
        return pl.ds(pl.multiple_of((side * pieces + k) * tile, tile), tile)

    def project(k):
        for side, to in ((1 - core, away), (core, own)):
            out = jnp.dot(ft_v[...], x_v[:, tokens_of(side, k)], preferred_element_type=F32)
            for g in range(groups):
                to[g, k] = out[g * group_rows : (g + 1) * group_rows, :]
            if to is away:
                sib_copy(k).start()

    ahead = min(2, pieces)
    for k in range(ahead):
        project(k)

    key_acc[...] = jnp.zeros_like(key_acc)
    value_acc[...] = jnp.zeros_like(value_acc)
    span = math.gcd(width, VALUE_DIM)

    def value_cotangent(side, k):
        for b in range(width // span):
            row_lambda = lambdas[(tp * width + b * span) // VALUE_DIM]
            at = (slice(b * span, (b + 1) * span), tokens_of(side, k))
            vc_v[at] = (vc_v[at].astype(F32) - row_lambda * sm_v[at].astype(F32)).astype(BF16)

    def accumulate(g, side, k):
        cols = tokens_of(side, k)
        piece = proj[g, side * pieces + k]
        dims = (((1,), (1,)), ((), ()))
        key_acc[g] += lax.dot_general(piece, kc_v[:, cols], dims, preferred_element_type=F32)
        value_acc[g] += lax.dot_general(piece, vc_v[:, cols], dims, preferred_element_type=F32)

    def accumulate_sibling(s):
        proj_copy(s, 1 - core).wait_recv()
        accumulate(s // pieces, 1 - core, s % pieces)

    def part_copy(g, d):
        to = lax.rem(fs + d, n_fs)
        return pltpu.make_async_remote_copy(
            src_ref=part.at[g, to],
            dst_ref=part_in.at[g, d - 1],
            send_sem=part_s.at[g, d - 1],
            recv_sem=part_r.at[g, d - 1],
            device_id=(to, tp),
            device_id_type=MESH,
        )

    def send_part(g):
        for kv, acc in enumerate((key_acc, value_acc)):
            for j in range(n_fs):
                rows = pl.ds(j * group_fs, group_fs)
                lows = pl.ds(group_rows + j * group_fs, group_fs)
                part[g, j, kv] = (acc[g, rows, :] + acc[g, lows, :]) * scale
        for d in range(1, n_fs):
            part_copy(g, d).start()

    @pl.loop(0, steps + LAG * (n_z - 1))
    def _(i):
        @pl.when(i < pieces)
        def _():
            sib_copy(i).wait_recv()
            own[:, i] = own[:, i] + sib[:, i]

        s_left = i - LAG * z

        @pl.when(jnp.logical_and(s_left >= 0, s_left < steps))
        def _():
            total = own[s_left // pieces, s_left % pieces]

            @pl.when(z > 0)
            def _():
                left_copy(s_left).wait_recv()
                left[s_left] = left[s_left] + total

            @pl.when(z == 0)
            def _():
                left[s_left] = total

            @pl.when(z < n_z - 1)
            def _():
                left_copy(s_left).start()

        s_right = i - LAG * (n_z - 1 - z)

        @pl.when(jnp.logical_and(s_right >= 0, s_right < steps))
        def _():
            total = own[s_right // pieces, s_right % pieces]

            @pl.when(z < n_z - 1)
            def _():
                right_copy(s_right).wait_recv()

                @pl.when(z > 0)
                def _():
                    right_out[s_right] = right[s_right] + total

            @pl.when(z == n_z - 1)
            def _():
                right[s_right] = jnp.zeros_like(total)

                @pl.when(z > 0)
                def _():
                    right_out[s_right] = total

            @pl.when(z > 0)
            def _():
                right_copy(s_right).start()

        @pl.when(i + ahead < pieces)
        def _():
            project(i + ahead)

        @pl.when(i == 0)
        def _():
            for load in loads[2:5]:
                load.wait()

        @pl.when(i < pieces)
        def _():
            for side in range(CORES):
                value_cotangent(side, i)

        s_done = i - LAG * jnp.maximum(z, n_z - 1 - z)

        @pl.when(jnp.logical_and(s_done >= 0, s_done < steps))
        def _():
            g = s_done // pieces
            mine = core * pieces + s_done % pieces
            high, low = split(left[s_done] + right[s_done])
            proj[g, mine, 0:group_rows, :] = high
            proj[g, mine, group_rows : 2 * group_rows, :] = low
            proj_copy(s_done, core).start()

            @pl.when(s_done > 0)
            def _():
                accumulate_sibling(s_done - 1)

            @pl.when(jnp.logical_and(s_done > 0, s_done % pieces == 0))
            def _():
                send_part(g - 1)

            accumulate(g, core, s_done % pieces)

        for t in range(1, bits):

            @pl.when(i == (steps * t) // bits)
            def _():
                wait_masters(t - 1)
                for j in range(1, 1 << t):
                    for kv in range(2):
                        master_copy(kv, t, j).start()

    accumulate_sibling(steps - 1)
    send_part(groups - 1)

    def dir_copy(g, d, source):
        at = dirs.at[g, source]
        return pltpu.make_async_remote_copy(
            src_ref=at,
            dst_ref=at,
            send_sem=dir_s.at[g, d - 1],
            recv_sem=dir_r.at[g, d - 1],
            device_id=(lax.rem(fs + d, n_fs), tp),
            device_id_type=MESH,
        )

    def norm_copy(d):
        return pltpu.make_async_remote_copy(
            src_ref=norms.at[0],
            dst_ref=norms.at[d],
            send_sem=norm_s.at[d - 1],
            recv_sem=norm_r.at[d - 1],
            device_id=(fs, lax.rem(tp + d, n_tp)),
            device_id_type=MESH,
        )

    for load in loads[5:]:
        load.wait()
    for g in range(groups):
        small = part[g, fs]
        for d in range(1, n_fs):
            part_copy(g, d).wait_recv()
            small = small + part_in[g, d - 1]
        rows = slice(g * group_fs, (g + 1) * group_fs)
        first_new = 0.8 * mom_v[0:2, rows] + 0.2 * small
        second_new = 0.9 * mom_v[2:4, rows] + 0.1 * small * small
        dirs[g, fs] = first_new / (jnp.sqrt(second_new) + 1e-06)
        for d in range(1, n_fs):
            dir_copy(g, d, fs).start()
        moved[0:2, rows] = first_new
        moved[2:4, rows] = second_new
    moments = pltpu.make_async_copy(moved, moved_out, out_sem.at[0])
    moments.start()
    for g in range(groups):
        for d in range(1, n_fs):
            dir_copy(g, d, lax.rem(fs + n_fs - d, n_fs)).wait_recv()

    block = fs_rows

    def raw_copy(kv, n):
        return pltpu.make_async_copy(raw.at[kv, n], raw_out.at[kv, n], out_sem.at[2 + kv * n_fs + n])

    sums = []
    for kv in range(2):
        high, low = split(jnp.concatenate(
            [dirs[g, j, kv] for j in range(n_fs) for g in range(groups)], axis=0
        ))

        def body(n, total):
            rows = fac_v[pl.ds(pl.multiple_of(n * block, block), block), :]
            out = jnp.dot(rows, high, preferred_element_type=F32) + jnp.dot(
                rows, low, preferred_element_type=F32
            )
            raw[kv, n] = out
            raw_copy(kv, n).start()
            return total + jnp.sum((out * out).reshape(block // 8, 8, width), axis=0)

        total = lax.fori_loop(0, n_fs, body, jnp.zeros((8, width), F32))
        sums.append(jnp.sum(total))
    norms[0, 0] = jnp.full(norms.shape[2:], sums[0], F32)
    norms[0, 1] = jnp.full(norms.shape[2:], sums[1], F32)
    for d in range(1, n_tp):
        norm_copy(d).start()
    wait_masters(bits - 1)
    squares = norms[0]
    for d in range(1, n_tp):
        norm_copy(d).wait_recv()
        squares = squares + norms[d]
    cells = factor.shape[0] * width * n_tp
    grain_v[...] = 0.02 / jnp.sqrt(squares / cells + 0.01)
    factors = pltpu.make_async_copy(grain_v, factors_out, out_sem.at[1])
    factors.start()

    @pl.loop(0, pieces)
    def _(k):
        sib_copy(k).wait_send()

    @pl.loop(0, steps)
    def _(s):
        proj_copy(s, core).wait_send()

        @pl.when(z < n_z - 1)
        def _():
            left_copy(s).wait_send()

        @pl.when(z > 0)
        def _():
            right_copy(s).wait_send()

    for kv in range(2):
        for step in range(bits):
            for j in range(1 << step):
                master_copy(kv, step, j).wait_send()
    for g in range(groups):
        for d in range(1, n_fs):
            part_copy(g, d).wait_send()
            dir_copy(g, d, fs).wait_send()
    for d in range(1, n_tp):
        norm_copy(d).wait_send()
    moments.wait()
    factors.wait()
    for kv in range(2):
        for n in range(n_fs):
            raw_copy(kv, n).wait()


def finish(
    n_fs,
    masters,
    raw,
    moved,
    factors,
    key_master,
    value_master,
    key_new,
    value_new,
    key_copy,
    value_copy,
    key_first_new,
    key_second_new,
    value_first_new,
    value_second_new,
    master_v,
    raw_v,
    copy_v,
    moved_v,
    in_sem,
    out_sem,
):
    fs = lax.axis_index("fs")
    block = key_master.shape[0]

    def own_in(kv):
        src = (key_master, value_master)[kv]
        return pltpu.make_async_copy(src, master_v.at[kv, fs], in_sem.at[0, kv, fs])

    def master_in(kv, n):
        return pltpu.make_async_copy(masters.at[kv, n], master_v.at[kv, n], in_sem.at[0, kv, n])

    def raw_in(kv, n):
        return pltpu.make_async_copy(raw.at[kv, n], raw_v.at[kv, n], in_sem.at[1, kv, n])

    moved_in = pltpu.make_async_copy(moved, moved_v, out_sem.at[0])
    for kv in range(2):
        for n in range(n_fs):

            @pl.when(fs == n)
            def _():
                own_in(kv).start()

            @pl.when(fs != n)
            def _():
                master_in(kv, n).start()

            raw_in(kv, n).start()
    moved_in.start()
    outs = []
    for kv in range(2):
        grain = factors[kv, 0:1, 0:1]
        for n in range(n_fs):
            master_in(kv, n).wait()
            raw_in(kv, n).wait()
            new = 0.998 * master_v[kv, n] - grain * raw_v[kv, n]
            copy_v[kv, n] = new.astype(BF16)
            to = (key_copy, value_copy)[kv].at[pl.ds(n * block, block), :]
            outs.append(pltpu.make_async_copy(copy_v.at[kv, n], to, in_sem.at[2, kv, n]))
            outs[-1].start()

            @pl.when(fs == n)
            def _():
                raw_v[kv, n] = new

        to = (key_new, value_new)[kv]
        outs.append(pltpu.make_async_copy(raw_v.at[kv, fs], to, out_sem.at[1 + kv]))
        outs[-1].start()
    moved_in.wait()
    for n, ref in enumerate((key_first_new, value_first_new, key_second_new, value_second_new)):
        outs.append(pltpu.make_async_copy(moved_v.at[n], ref, out_sem.at[3 + n]))
        outs[-1].start()
    for out in outs:
        out.wait()


def local(n_fs, n_tp, *args):
    normed, key_cot, first_map, second_map, lambdas, factor, key_master = args[:7]
    features, tokens = normed.shape
    width = first_map.shape[0]
    rows, rank = factor.shape
    fs_rows = key_master.shape[0]
    rank_rows = rank // n_fs
    tile = TOKENS_AT_ONCE
    pieces = tokens // (CORES * tile)
    groups = max(1, min(4, rank_rows // 8))
    group_rows = rank // groups
    group_fs = rank_rows // groups
    steps = groups * pieces
    gathered = (2, n_fs, fs_rows, width)
    scale = 1.0 / math.sqrt(tokens * n_fs)
    any_spec = pl.BlockSpec(memory_space=pl.ANY)
    specs = [any_spec] * 12
    specs[4] = pl.BlockSpec(memory_space=pltpu.SMEM)
    dma = pltpu.SemaphoreType.DMA
    sds = jax.ShapeDtypeStruct
    small = sds((rank_rows, width), F32)
    masters, raw, moved, factors = pl.pallas_call(
        functools.partial(kernel, n_fs, n_tp, scale),
        out_shape=[
            sds(gathered, F32),
            sds(gathered, F32),
            sds((4, rank_rows, width), F32),
            sds((2, 8, LANES), F32),
        ],
        in_specs=specs,
        out_specs=[any_spec] * 4,
        scratch_shapes=[
            pltpu.VMEM((features, tokens), BF16),
            pltpu.VMEM((width, tokens), BF16),
            pltpu.VMEM((width, tokens), BF16),
            pltpu.VMEM((width, tokens), BF16),
            pltpu.VMEM((rows, rank), BF16),
            pltpu.VMEM((rank, features), F32),
            pltpu.VMEM((rank, features), BF16),
            pltpu.VMEM((4, rank_rows, width), F32),
            pltpu.VMEM((groups, pieces, group_rows, tile), F32),
            pltpu.VMEM((groups, pieces, group_rows, tile), F32),
            pltpu.VMEM((groups, pieces, group_rows, tile), F32),
            pltpu.VMEM((steps, group_rows, tile), F32),
            pltpu.VMEM((steps, group_rows, tile), F32),
            pltpu.VMEM((steps, group_rows, tile), F32),
            pltpu.VMEM((groups, CORES * pieces, 2 * group_rows, tile), BF16),
            pltpu.VMEM((groups, 2 * group_rows, width), F32),
            pltpu.VMEM((groups, 2 * group_rows, width), F32),
            pltpu.VMEM(gathered, F32),
            pltpu.VMEM((2, 8, LANES), F32),
            pltpu.VMEM((groups, n_fs, 2, group_fs, width), F32),
            pltpu.VMEM((groups, n_fs - 1, 2, group_fs, width), F32),
            pltpu.VMEM((4, rank_rows, width), F32),
            pltpu.VMEM((groups, n_fs, 2, group_fs, width), F32),
            pltpu.VMEM((n_tp, 2, 8, LANES), F32),
            dma((9,)),
            dma((pieces,)),
            dma((pieces,)),
            dma((steps,)),
            dma((steps,)),
            dma((steps,)),
            dma((steps,)),
            dma((steps,)),
            dma((steps,)),
            dma((2, n_fs - 1)),
            dma((2, n_fs - 1)),
            dma((groups, n_fs - 1)),
            dma((groups, n_fs - 1)),
            dma((groups, n_fs - 1)),
            dma((groups, n_fs - 1)),
            dma((n_tp - 1,)),
            dma((n_tp - 1,)),
            dma((2 + 2 * n_fs,)),
        ],
        compiler_params=pltpu.CompilerParams(
            collective_id=0, has_side_effects=True, vmem_limit_bytes=40 * 1024 * 1024
        ),
    )(*args)
    vmem_spec = pl.BlockSpec(memory_space=pltpu.VMEM)
    return pl.pallas_call(
        functools.partial(finish, n_fs),
        out_shape=[
            sds((fs_rows, width), F32),
            sds((fs_rows, width), F32),
            sds((rows, width), BF16),
            sds((rows, width), BF16),
            small,
            small,
            small,
            small,
        ],
        in_specs=[any_spec, any_spec, any_spec, vmem_spec, any_spec, any_spec],
        out_specs=[any_spec] * 8,
        scratch_shapes=[
            pltpu.VMEM(gathered, F32),
            pltpu.VMEM(gathered, F32),
            pltpu.VMEM(gathered, BF16),
            pltpu.VMEM((4, rank_rows, width), F32),
            dma((3, 2, n_fs)),
            dma((7,)),
        ],
        compiler_params=pltpu.CompilerParams(vmem_limit_bytes=20 * 1024 * 1024),
    )(masters, raw, moved, factors, key_master, args[7])


def solution(mesh):
    in_specs = (
        P("tp", "fs"),
        P("tp", "fs"),
        P("tp", "fs"),
        P("tp", "fs"),
        P(),
        P(),
        P("fs", "tp"),
        P("fs", "tp"),
        P("fs", "tp"),
        P("fs", "tp"),
        P("fs", "tp"),
        P("fs", "tp"),
    )
    out_specs = (
        P("fs", "tp"),
        P("fs", "tp"),
        P(None, "tp"),
        P(None, "tp"),
        P("fs", "tp"),
        P("fs", "tp"),
        P("fs", "tp"),
        P("fs", "tp"),
    )
    body = functools.partial(local, mesh.shape["fs"], mesh.shape["tp"])

    def ordered(*args):
        out = body(*args)
        return tuple(out)

    return jax.shard_map(ordered, mesh=mesh, in_specs=in_specs, out_specs=out_specs, check_vma=False)
```

```python
import functools
import math

import jax
import jax.numpy as jnp
from jax import lax
from jax.experimental import pallas as pl
from jax.experimental.pallas import tpu as pltpu
from jax.sharding import PartitionSpec as P

VALUE_DIM = 256
CORES = 2
LANES = 128
TOKENS_AT_ONCE = 256
LAG = 3
MESH = pl.DeviceIdType.MESH
F32 = jnp.float32
BF16 = jnp.bfloat16


def flipped(index, bit):
    step = 1 << bit
    return index + step * (1 - 2 * ((index // step) % 2))


def split(value):
    high = value.astype(BF16)
    return high, (value - high.astype(F32)).astype(BF16)


def kernel(
    n_fs,
    n_tp,
    scale,
    normed,
    key_cot,
    first_map,
    second_map,
    lambdas,
    factor,
    key_master,
    value_master,
    key_first,
    key_second,
    value_first,
    value_second,
    masters,
    raw_out,
    moved_out,
    factors_out,
    x_v,
    kc_v,
    vc_v,
    sm_v,
    fac_v,
    ft32,
    ft_v,
    mom_v,
    own,
    away,
    sib,
    left,
    right,
    right_out,
    proj,
    key_acc,
    value_acc,
    raw,
    grain_v,
    part,
    part_in,
    moved,
    dirs,
    norms,
    in_sem,
    sib_s,
    sib_r,
    left_s,
    left_r,
    right_s,
    right_r,
    proj_s,
    proj_r,
    mast_s,
    mast_r,
    part_s,
    part_r,
    dir_s,
    dir_r,
    norm_s,
    norm_r,
    out_sem,
):
    fs = lax.axis_index("fs")
    tp = lax.axis_index("tp")
    z = tp // CORES
    core = tp % CORES
    n_z = n_tp // CORES
    features = normed.shape[0]
    width = first_map.shape[0]
    rank = factor.shape[1]
    groups, pieces, group_rows, tile = own.shape
    steps = groups * pieces
    group_fs = group_rows // n_fs
    fs_rows = key_master.shape[0]
    rank_rows = rank // n_fs
    bits = n_fs.bit_length() - 1
    other = z * CORES + (1 - core)

    loads = [
        pltpu.make_async_copy(normed, x_v, in_sem.at[0]),
        pltpu.make_async_copy(factor, fac_v, in_sem.at[1]),
        pltpu.make_async_copy(first_map, vc_v, in_sem.at[2]),
        pltpu.make_async_copy(second_map, sm_v, in_sem.at[3]),
        pltpu.make_async_copy(key_cot, kc_v, in_sem.at[4]),
        pltpu.make_async_copy(key_first, mom_v.at[0], in_sem.at[5]),
        pltpu.make_async_copy(value_first, mom_v.at[1], in_sem.at[6]),
        pltpu.make_async_copy(key_second, mom_v.at[2], in_sem.at[7]),
        pltpu.make_async_copy(value_second, mom_v.at[3], in_sem.at[8]),
    ]
    for load in loads:
        load.start()

    barrier = pltpu.get_barrier_semaphore()
    for d in range(1, n_fs):
        pl.semaphore_signal(
            barrier, inc=1, device_id=(lax.rem(fs + d, n_fs), tp), device_id_type=MESH
        )
    for d in range(1, n_tp):
        pl.semaphore_signal(
            barrier, inc=1, device_id=(fs, lax.rem(tp + d, n_tp)), device_id_type=MESH
        )
    pl.semaphore_wait(barrier, n_fs + n_tp - 2)

    def master_copy(kv, step, j):
        order = list(range(bits)) if kv == 0 else list(range(bits))[::-1]
        block = fs
        for t in range(step):
            if (j >> t) & 1:
                block = flipped(block, order[t])
        if j == 0:
            src = (key_master, value_master)[kv]
        else:
            src = masters.at[kv, block]
        slot = (1 << step) - 1 + j
        return pltpu.make_async_remote_copy(
            src_ref=src,
            dst_ref=masters.at[kv, block],
            send_sem=mast_s.at[kv, slot],
            recv_sem=mast_r.at[kv, slot],
            device_id=(flipped(fs, order[step]), tp),
            device_id_type=MESH,
        )

    for step in range(bits):
        for kv in range(2):
            master_copy(kv, step, 0).start()

    def wait_masters(step):
        for kv in range(2):
            for j in range(1 << step):
                master_copy(kv, step, j).wait_recv()

    def sib_copy(k):
        return pltpu.make_async_remote_copy(
            src_ref=away.at[:, k],
            dst_ref=sib.at[:, k],
            send_sem=sib_s.at[k],
            recv_sem=sib_r.at[k],
            device_id=(fs, other),
            device_id_type=MESH,
        )

    def left_copy(s):
        return pltpu.make_async_remote_copy(
            src_ref=left.at[s],
            dst_ref=left.at[s],
            send_sem=left_s.at[s],
            recv_sem=left_r.at[s],
            device_id=(fs, lax.rem(tp + CORES, n_tp)),
            device_id_type=MESH,
        )

    def right_copy(s):
        return pltpu.make_async_remote_copy(
            src_ref=right_out.at[s],
            dst_ref=right.at[s],
            send_sem=right_s.at[s],
            recv_sem=right_r.at[s],
            device_id=(fs, lax.rem(tp + n_tp - CORES, n_tp)),
            device_id_type=MESH,
        )

    def proj_copy(s, side):
        at = proj.at[s // pieces, side * pieces + s % pieces]
        return pltpu.make_async_remote_copy(
            src_ref=at,
            dst_ref=at,
            send_sem=proj_s.at[s],
            recv_sem=proj_r.at[s],
            device_id=(fs, other),
            device_id_type=MESH,
        )

    loads[0].wait()
    loads[1].wait()
    turned = fac_v[pl.ds(pl.multiple_of(tp * features, features), features), :].astype(F32).T
    for g in range(groups):
        for j in range(n_fs):
            row = j * rank_rows + g * group_fs
            at = g * group_rows + j * group_fs
            ft32[at : at + group_fs, :] = turned[row : row + group_fs, :]
    ft_v[...] = ft32[...].astype(BF16)

    def tokens_of(side, k):
        return pl.ds(pl.multiple_of((side * pieces + k) * tile, tile), tile)

    def project(k):
        for side, to in ((1 - core, away), (core, own)):
            out = jnp.dot(ft_v[...], x_v[:, tokens_of(side, k)], preferred_element_type=F32)
            for g in range(groups):
                to[g, k] = out[g * group_rows : (g + 1) * group_rows, :]
            if to is away:
                sib_copy(k).start()

    ahead = min(2, pieces)
    for k in range(ahead):
        project(k)

    key_acc[...] = jnp.zeros_like(key_acc)
    value_acc[...] = jnp.zeros_like(value_acc)
    span = math.gcd(width, VALUE_DIM)

    def value_cotangent(side, k):
        for b in range(width // span):
            row_lambda = lambdas[(tp * width + b * span) // VALUE_DIM]
            at = (slice(b * span, (b + 1) * span), tokens_of(side, k))
            vc_v[at] = (vc_v[at].astype(F32) - row_lambda * sm_v[at].astype(F32)).astype(BF16)

    def accumulate(g, side, k):
        cols = tokens_of(side, k)
        piece = proj[g, side * pieces + k]
        dims = (((1,), (1,)), ((), ()))
        key_acc[g] += lax.dot_general(piece, kc_v[:, cols], dims, preferred_element_type=F32)
        value_acc[g] += lax.dot_general(piece, vc_v[:, cols], dims, preferred_element_type=F32)

    def accumulate_sibling(s):
        proj_copy(s, 1 - core).wait_recv()
        accumulate(s // pieces, 1 - core, s % pieces)

    def part_copy(g, d):
        to = lax.rem(fs + d, n_fs)
        return pltpu.make_async_remote_copy(
            src_ref=part.at[g, to],
            dst_ref=part_in.at[g, d - 1],
            send_sem=part_s.at[g, d - 1],
            recv_sem=part_r.at[g, d - 1],
            device_id=(to, tp),
            device_id_type=MESH,
        )

    def send_part(g):
        for kv, acc in enumerate((key_acc, value_acc)):
            for j in range(n_fs):
                rows = pl.ds(j * group_fs, group_fs)
                lows = pl.ds(group_rows + j * group_fs, group_fs)
                part[g, j, kv] = (acc[g, rows, :] + acc[g, lows, :]) * scale
        for d in range(1, n_fs):
            part_copy(g, d).start()

    @pl.loop(0, steps + LAG * (n_z - 1))
    def _(i):
        @pl.when(i < pieces)
        def _():
            sib_copy(i).wait_recv()
            own[:, i] = own[:, i] + sib[:, i]

        s_left = i - LAG * z

        @pl.when(jnp.logical_and(s_left >= 0, s_left < steps))
        def _():
            total = own[s_left // pieces, s_left % pieces]

            @pl.when(z > 0)
            def _():
                left_copy(s_left).wait_recv()
                left[s_left] = left[s_left] + total

            @pl.when(z == 0)
            def _():
                left[s_left] = total

            @pl.when(z < n_z - 1)
            def _():
                left_copy(s_left).start()

        s_right = i - LAG * (n_z - 1 - z)

        @pl.when(jnp.logical_and(s_right >= 0, s_right < steps))
        def _():
            total = own[s_right // pieces, s_right % pieces]

            @pl.when(z < n_z - 1)
            def _():
                right_copy(s_right).wait_recv()

                @pl.when(z > 0)
                def _():
                    right_out[s_right] = right[s_right] + total

            @pl.when(z == n_z - 1)
            def _():
                right[s_right] = jnp.zeros_like(total)

                @pl.when(z > 0)
                def _():
                    right_out[s_right] = total

            @pl.when(z > 0)
            def _():
                right_copy(s_right).start()

        @pl.when(i + ahead < pieces)
        def _():
            project(i + ahead)

        @pl.when(i == 0)
        def _():
            for load in loads[2:5]:
                load.wait()

        @pl.when(i < pieces)
        def _():
            for side in range(CORES):
                value_cotangent(side, i)

        s_done = i - LAG * jnp.maximum(z, n_z - 1 - z)

        @pl.when(jnp.logical_and(s_done >= 0, s_done < steps))
        def _():
            g = s_done // pieces
            mine = core * pieces + s_done % pieces
            high, low = split(left[s_done] + right[s_done])
            proj[g, mine, 0:group_rows, :] = high
            proj[g, mine, group_rows : 2 * group_rows, :] = low
            proj_copy(s_done, core).start()

            @pl.when(s_done > 0)
            def _():
                accumulate_sibling(s_done - 1)

            @pl.when(jnp.logical_and(s_done > 0, s_done % pieces == 0))
            def _():
                send_part(g - 1)

            accumulate(g, core, s_done % pieces)

        for t in range(1, bits):

            @pl.when(i == (steps * t) // bits)
            def _():
                wait_masters(t - 1)
                for j in range(1, 1 << t):
                    for kv in range(2):
                        master_copy(kv, t, j).start()

    accumulate_sibling(steps - 1)
    send_part(groups - 1)

    def dir_copy(g, d, source):
        at = dirs.at[g, source]
        return pltpu.make_async_remote_copy(
            src_ref=at,
            dst_ref=at,
            send_sem=dir_s.at[g, d - 1],
            recv_sem=dir_r.at[g, d - 1],
            device_id=(lax.rem(fs + d, n_fs), tp),
            device_id_type=MESH,
        )

    def norm_copy(d):
        return pltpu.make_async_remote_copy(
            src_ref=norms.at[0],
            dst_ref=norms.at[d],
            send_sem=norm_s.at[d - 1],
            recv_sem=norm_r.at[d - 1],
            device_id=(fs, lax.rem(tp + d, n_tp)),
            device_id_type=MESH,
        )

    for load in loads[5:]:
        load.wait()
    for g in range(groups):
        small = part[g, fs]
        for d in range(1, n_fs):
            part_copy(g, d).wait_recv()
            small = small + part_in[g, d - 1]
        rows = slice(g * group_fs, (g + 1) * group_fs)
        first_new = 0.8 * mom_v[0:2, rows] + 0.2 * small
        second_new = 0.9 * mom_v[2:4, rows] + 0.1 * small * small
        dirs[g, fs] = first_new / (jnp.sqrt(second_new) + 1e-06)
        for d in range(1, n_fs):
            dir_copy(g, d, fs).start()
        moved[0:2, rows] = first_new
        moved[2:4, rows] = second_new
    moments = pltpu.make_async_copy(moved, moved_out, out_sem.at[0])
    moments.start()
    for g in range(groups):
        for d in range(1, n_fs):
            dir_copy(g, d, lax.rem(fs + n_fs - d, n_fs)).wait_recv()

    block = fs_rows

    def raw_copy(kv, n):
        return pltpu.make_async_copy(raw.at[kv, n], raw_out.at[kv, n], out_sem.at[2 + kv * n_fs + n])

    sums = []
    for kv in range(2):
        high, low = split(jnp.concatenate(
            [dirs[g, j, kv] for j in range(n_fs) for g in range(groups)], axis=0
        ))

        def body(n, total):
            rows = fac_v[pl.ds(pl.multiple_of(n * block, block), block), :]
            out = jnp.dot(rows, high, preferred_element_type=F32) + jnp.dot(
                rows, low, preferred_element_type=F32
            )
            raw[kv, n] = out
            raw_copy(kv, n).start()
            return total + jnp.sum((out * out).reshape(block // 8, 8, width), axis=0)

        total = lax.fori_loop(0, n_fs, body, jnp.zeros((8, width), F32))
        sums.append(jnp.sum(total))
    norms[0, 0] = jnp.full(norms.shape[2:], sums[0], F32)
    norms[0, 1] = jnp.full(norms.shape[2:], sums[1], F32)
    for d in range(1, n_tp):
        norm_copy(d).start()
    wait_masters(bits - 1)
    squares = norms[0]
    for d in range(1, n_tp):
        norm_copy(d).wait_recv()
        squares = squares + norms[d]
    cells = factor.shape[0] * width * n_tp
    grain_v[...] = 0.02 / jnp.sqrt(squares / cells + 0.01)
    factors = pltpu.make_async_copy(grain_v, factors_out, out_sem.at[1])
    factors.start()

    @pl.loop(0, pieces)
    def _(k):
        sib_copy(k).wait_send()

    @pl.loop(0, steps)
    def _(s):
        proj_copy(s, core).wait_send()

        @pl.when(z < n_z - 1)
        def _():
            left_copy(s).wait_send()

        @pl.when(z > 0)
        def _():
            right_copy(s).wait_send()

    for kv in range(2):
        for step in range(bits):
            for j in range(1 << step):
                master_copy(kv, step, j).wait_send()
    for g in range(groups):
        for d in range(1, n_fs):
            part_copy(g, d).wait_send()
            dir_copy(g, d, fs).wait_send()
    for d in range(1, n_tp):
        norm_copy(d).wait_send()
    moments.wait()
    factors.wait()
    for kv in range(2):
        for n in range(n_fs):
            raw_copy(kv, n).wait()


def finish(
    n_fs,
    masters,
    raw,
    moved,
    factors,
    key_master,
    value_master,
    key_new,
    value_new,
    key_copy,
    value_copy,
    key_first_new,
    key_second_new,
    value_first_new,
    value_second_new,
    master_v,
    raw_v,
    copy_v,
    moved_v,
    in_sem,
    out_sem,
):
    fs = lax.axis_index("fs")
    block = key_master.shape[0]

    def own_in(kv):
        src = (key_master, value_master)[kv]
        return pltpu.make_async_copy(src, master_v.at[kv, fs], in_sem.at[0, kv, fs])

    def master_in(kv, n):
        return pltpu.make_async_copy(masters.at[kv, n], master_v.at[kv, n], in_sem.at[0, kv, n])

    def raw_in(kv, n):
        return pltpu.make_async_copy(raw.at[kv, n], raw_v.at[kv, n], in_sem.at[1, kv, n])

    moved_in = pltpu.make_async_copy(moved, moved_v, out_sem.at[0])
    for kv in range(2):
        for n in range(n_fs):

            @pl.when(fs == n)
            def _():
                own_in(kv).start()

            @pl.when(fs != n)
            def _():
                master_in(kv, n).start()

            raw_in(kv, n).start()
    moved_in.start()
    outs = []
    for kv in range(2):
        grain = factors[kv, 0:1, 0:1]
        for n in range(n_fs):
            master_in(kv, n).wait()
            raw_in(kv, n).wait()
            new = 0.998 * master_v[kv, n] - grain * raw_v[kv, n]
            copy_v[kv, n] = new.astype(BF16)
            to = (key_copy, value_copy)[kv].at[pl.ds(n * block, block), :]
            outs.append(pltpu.make_async_copy(copy_v.at[kv, n], to, in_sem.at[2, kv, n]))
            outs[-1].start()

            @pl.when(fs == n)
            def _():
                raw_v[kv, n] = new

        to = (key_new, value_new)[kv]
        outs.append(pltpu.make_async_copy(raw_v.at[kv, fs], to, out_sem.at[1 + kv]))
        outs[-1].start()
    moved_in.wait()
    for n, ref in enumerate((key_first_new, value_first_new, key_second_new, value_second_new)):
        outs.append(pltpu.make_async_copy(moved_v.at[n], ref, out_sem.at[3 + n]))
        outs[-1].start()
    for out in outs:
        out.wait()


def local(n_fs, n_tp, *args):
    normed, key_cot, first_map, second_map, lambdas, factor, key_master = args[:7]
    features, tokens = normed.shape
    width = first_map.shape[0]
    rows, rank = factor.shape
    fs_rows = key_master.shape[0]
    rank_rows = rank // n_fs
    tile = TOKENS_AT_ONCE
    pieces = tokens // (CORES * tile)
    groups = max(1, min(4, rank_rows // 8))
    group_rows = rank // groups
    group_fs = rank_rows // groups
    steps = groups * pieces
    gathered = (2, n_fs, fs_rows, width)
    scale = 1.0 / math.sqrt(tokens * n_fs)
    any_spec = pl.BlockSpec(memory_space=pl.ANY)
    specs = [any_spec] * 12
    specs[4] = pl.BlockSpec(memory_space=pltpu.SMEM)
    dma = pltpu.SemaphoreType.DMA
    sds = jax.ShapeDtypeStruct
    small = sds((rank_rows, width), F32)
    masters, raw, moved, factors = pl.pallas_call(
        functools.partial(kernel, n_fs, n_tp, scale),
        out_shape=[
            sds(gathered, F32),
            sds(gathered, F32),
            sds((4, rank_rows, width), F32),
            sds((2, 8, LANES), F32),
        ],
        in_specs=specs,
        out_specs=[any_spec] * 4,
        scratch_shapes=[
            pltpu.VMEM((features, tokens), BF16),
            pltpu.VMEM((width, tokens), BF16),
            pltpu.VMEM((width, tokens), BF16),
            pltpu.VMEM((width, tokens), BF16),
            pltpu.VMEM((rows, rank), BF16),
            pltpu.VMEM((rank, features), F32),
            pltpu.VMEM((rank, features), BF16),
            pltpu.VMEM((4, rank_rows, width), F32),
            pltpu.VMEM((groups, pieces, group_rows, tile), F32),
            pltpu.VMEM((groups, pieces, group_rows, tile), F32),
            pltpu.VMEM((groups, pieces, group_rows, tile), F32),
            pltpu.VMEM((steps, group_rows, tile), F32),
            pltpu.VMEM((steps, group_rows, tile), F32),
            pltpu.VMEM((steps, group_rows, tile), F32),
            pltpu.VMEM((groups, CORES * pieces, 2 * group_rows, tile), BF16),
            pltpu.VMEM((groups, 2 * group_rows, width), F32),
            pltpu.VMEM((groups, 2 * group_rows, width), F32),
            pltpu.VMEM(gathered, F32),
            pltpu.VMEM((2, 8, LANES), F32),
            pltpu.VMEM((groups, n_fs, 2, group_fs, width), F32),
            pltpu.VMEM((groups, n_fs - 1, 2, group_fs, width), F32),
            pltpu.VMEM((4, rank_rows, width), F32),
            pltpu.VMEM((groups, n_fs, 2, group_fs, width), F32),
            pltpu.VMEM((n_tp, 2, 8, LANES), F32),
            dma((9,)),
            dma((pieces,)),
            dma((pieces,)),
            dma((steps,)),
            dma((steps,)),
            dma((steps,)),
            dma((steps,)),
            dma((steps,)),
            dma((steps,)),
            dma((2, n_fs - 1)),
            dma((2, n_fs - 1)),
            dma((groups, n_fs - 1)),
            dma((groups, n_fs - 1)),
            dma((groups, n_fs - 1)),
            dma((groups, n_fs - 1)),
            dma((n_tp - 1,)),
            dma((n_tp - 1,)),
            dma((2 + 2 * n_fs,)),
        ],
        compiler_params=pltpu.CompilerParams(
            collective_id=0, has_side_effects=True, vmem_limit_bytes=63 * 1024 * 1024
        ),
    )(*args)
    vmem_spec = pl.BlockSpec(memory_space=pltpu.VMEM)
    return pl.pallas_call(
        functools.partial(finish, n_fs),
        out_shape=[
            sds((fs_rows, width), F32),
            sds((fs_rows, width), F32),
            sds((rows, width), BF16),
            sds((rows, width), BF16),
            small,
            small,
            small,
            small,
        ],
        in_specs=[any_spec, any_spec, any_spec, vmem_spec, any_spec, any_spec],
        out_specs=[any_spec] * 8,
        scratch_shapes=[
            pltpu.VMEM(gathered, F32),
            pltpu.VMEM(gathered, F32),
            pltpu.VMEM(gathered, BF16),
            pltpu.VMEM((4, rank_rows, width), F32),
            dma((3, 2, n_fs)),
            dma((7,)),
        ],
        compiler_params=pltpu.CompilerParams(vmem_limit_bytes=63 * 1024 * 1024),
    )(masters, raw, moved, factors, key_master, args[7])


def solution(mesh):
    in_specs = (
        P("tp", "fs"),
        P("tp", "fs"),
        P("tp", "fs"),
        P("tp", "fs"),
        P(),
        P(),
        P("fs", "tp"),
        P("fs", "tp"),
        P("fs", "tp"),
        P("fs", "tp"),
        P("fs", "tp"),
        P("fs", "tp"),
    )
    out_specs = (
        P("fs", "tp"),
        P("fs", "tp"),
        P(None, "tp"),
        P(None, "tp"),
        P("fs", "tp"),
        P("fs", "tp"),
        P("fs", "tp"),
        P("fs", "tp"),
    )
    body = functools.partial(local, mesh.shape["fs"], mesh.shape["tp"])

    def ordered(*args):
        out = body(*args)
        return tuple(out)

    return jax.shard_map(ordered, mesh=mesh, in_specs=in_specs, out_specs=out_specs, check_vma=False)
```
